512 devices in a mesh: grp: 2 (over y), sp: 32 (over z), tp: 8 (over x, core).
Axes of the slice: x: 4, y: 2, z: 32, core: 2. Of those that a mesh axis runs over, the one named last changes fastest.
The devices are a block of a 4x8x32 slice.
Arguments:
- tokens: bfloat16 [24576, 2048], P(('grp', 'sp'), 'tp'), parts along dimension 0, may hold values from -6 to 6
- norm_gain: float32 [2048], replicated, may hold values from 0.1 to 1.9
- qk_gain: float32 [4, 64], replicated, may hold values from 0.7 to 5.5
- w_query_window: bfloat16 [2048, 1024], P('sp', 'tp'), may hold values from -1 to 1
- w_key_window: bfloat16 [2048, 512], P('sp', 'tp'), may hold values from -1 to 1
- w_value_window: bfloat16 [2048, 512], P('sp', 'tp'), may hold values from -0.125 to 0.125
- sink_logits: float32 [16], P('tp'), may hold values from 0 to 5
- w_query_forget: bfloat16 [2048, 1024], P('sp', 'tp'), may hold values from -1 to 1
- w_key_forget: bfloat16 [2048, 1024], P('sp', 'tp'), may hold values from -1 to 1
- w_value_forget: bfloat16 [2048, 1024], P('sp', 'tp'), may hold values from -0.125 to 0.125
- gate_cum: float32 [24576, 16], P(('grp', 'sp'), 'tp'), parts along dimension 0, as said below
- w_merge: bfloat16 [2048, 2, 2048], P('sp', None, 'tp'), may hold values from -0.125 to 0.125
- w_branch: bfloat16 [2, 1024, 2048], P(None, 'sp', 'tp'), may hold values from -0.8984375 to 0.8984375
Outputs:
- mixed: bfloat16 [24576, 2048], P(('grp', 'sp'), 'tp'), parts along dimension 0
The draws below stay inside these ranges and needn't reach their ends.
There are 2 independent parts, one for each index of `grp`. The reference program is written for one: setup_inputs(seed, part) draws one part's arguments, and reference() takes and returns one part's arrays. A program takes and returns all parts, laid end to end along the dimension named above; an argument that names none is the same for every part. Nothing has to cross between parts.
Inputs may be any that keep to these rules, and one draw needn't show every extreme that they name: `gate_cum`: along positions each head's values never rise.
All inputs are finite; a program needn't handle non-finite values.
Results may differ from the reference program's by a relative error of at most 0.012.
Values may be sent and summed in bfloat16 or wider, within the bound.
A program may use at most 64 MiB of HBM per device.

```python
import math
import jax
import jax.numpy as jnp
from jax import lax

D = 2048
QUERY_HEAD_COUNT = 16
KV_HEADS = 8
HEAD = 64
WINDOW = 128
TOK_DEV = 384
SEQUENCE_LENGTH = 12288


def query_raw(key, offset_salt, col_count):
    return jax.random.normal(jax.random.fold_in(key, offset_salt), (D, col_count), jnp.float32) * D ** (-0.5)


def draw_qk_gain(key, part):
    gain_table = jax.random.uniform(jax.random.fold_in(key, 7), (4, HEAD), jnp.float32, 0.7, 1.3)
    return gain_table


def draw_w_query_window(key, part):
    return query_raw(key, 11, QUERY_HEAD_COUNT * HEAD).astype(jnp.bfloat16)


def draw_w_key_window(key, part):
    fresh_part = query_raw(key, 12, KV_HEADS * HEAD)
    return fresh_part.astype(jnp.bfloat16)


def draw_w_query_forget(key, part):
    return query_raw(key, 13, QUERY_HEAD_COUNT * HEAD).astype(jnp.bfloat16)


def draw_w_key_forget(key, part):
    fresh_part = query_raw(key, 14, QUERY_HEAD_COUNT * HEAD)
    return fresh_part.astype(jnp.bfloat16)


def draw_gate_cum(key, part):
    head_order = jax.random.permutation(jax.random.fold_in(key, 21), QUERY_HEAD_COUNT)
    lagging_heads = head_order < QUERY_HEAD_COUNT // 2
    slow_rate = jnp.exp(jax.random.uniform(jax.random.fold_in(key, 22), (QUERY_HEAD_COUNT,), jnp.float32, jnp.log(0.3), jnp.log(1.2))) / SEQUENCE_LENGTH
    fast_rate = jnp.exp(jax.random.uniform(jax.random.fold_in(key, 23), (QUERY_HEAD_COUNT,), jnp.float32, jnp.log(0.01), jnp.log(0.033)))
    step_rate = jnp.where(lagging_heads, slow_rate, fast_rate)
    block_factor = jnp.exp(jax.random.uniform(jax.random.fold_in(key, 24), (SEQUENCE_LENGTH // TOK_DEV, QUERY_HEAD_COUNT), jnp.float32, jnp.log(0.5), jnp.log(2.0)))
    block_factor = jnp.repeat(block_factor, TOK_DEV, axis=0)
    jitter = jax.random.uniform(jax.random.fold_in(key, 25), (SEQUENCE_LENGTH, QUERY_HEAD_COUNT), jnp.float32, 0.3, 1.7)
    step_count = -step_rate[None, :] * block_factor * jitter
    spike_locations = jax.random.randint(jax.random.fold_in(key, 26), (3,), 0, SEQUENCE_LENGTH)
    spike_misses = jnp.log(1.0 - jax.random.uniform(jax.random.fold_in(key, 27), (3, QUERY_HEAD_COUNT), jnp.float32, 0.2, 0.4))
    spike_matches = (jnp.arange(SEQUENCE_LENGTH)[:, None] == spike_locations[None, :]).astype(jnp.float32)
    spike_events = jnp.dot(spike_matches, spike_misses) * lagging_heads.astype(jnp.float32)[None, :]
    return jnp.cumsum(step_count + spike_events, axis=0)


def block_scale(own_key, shape, cuts, least, high):
    level = 1.0
    for position, shards_of in cuts:
        steps = jax.random.uniform(jax.random.fold_in(jax.random.fold_in(own_key, 6), position), (shards_of,), jnp.float32, least / len(cuts), high / len(cuts))
        level = level * jnp.repeat(jnp.exp(steps), shape[position] // shards_of).reshape((-1,) + (1,) * (len(shape) - 1 - position))
    return level


def scatter_about(own_key, dims, deviation, bound, cuts=(), kind=jnp.bfloat16):
    level = block_scale(own_key, dims, cuts, -0.22, 0.18) if cuts else 1.0
    array = jax.random.normal(own_key, dims, jnp.float32) * deviation * level
    return jnp.minimum(jnp.maximum(array, -bound), bound).astype(kind)


def setup_inputs(seed: int = 0, part: int = 0) -> dict:
    arg_keys = jax.random.split(jax.random.key(seed), 14)
    own_keys = jax.random.split(jax.random.fold_in(arg_keys[13], part), 14)
    tokens = scatter_about(own_keys[0], (SEQUENCE_LENGTH, D), 1.0, 6.0, ((0, 32), (1, 8)))
    norm_gain = jnp.clip(1.0 + 0.18 * jax.random.normal(arg_keys[1], (D,), jnp.float32), 0.1, 1.9)
    qk_gain = draw_qk_gain(jax.random.fold_in(arg_keys[13], 71), part)
    w_query_window = draw_w_query_window(jax.random.fold_in(arg_keys[13], 71), part)
    w_key_window = draw_w_key_window(jax.random.fold_in(arg_keys[13], 71), part)
    w_value_window = scatter_about(arg_keys[5], (D, KV_HEADS * HEAD), D ** -0.5, 0.125, ((0, 32), (1, 8)))
    sink_logits = jnp.clip(5.0 * jax.random.uniform(arg_keys[6], (QUERY_HEAD_COUNT,), jnp.float32) ** block_scale(arg_keys[6], (QUERY_HEAD_COUNT,), ((0, 8),), -0.2, 0.2), 0.0, 5.0)
    w_query_forget = draw_w_query_forget(jax.random.fold_in(arg_keys[13], 71), part)
    w_key_forget = draw_w_key_forget(jax.random.fold_in(arg_keys[13], 71), part)
    w_value_forget = scatter_about(arg_keys[9], (D, QUERY_HEAD_COUNT * HEAD), D ** -0.5, 0.125, ((0, 32), (1, 8)))
    gate_cum = draw_gate_cum(jax.random.fold_in(jax.random.fold_in(arg_keys[13], part), 71), part)
    w_merge = scatter_about(arg_keys[11], (D, 2, D), D ** -0.5, 0.125, ((0, 32), (2, 8)))
    w_branch = scatter_about(arg_keys[12], (2, QUERY_HEAD_COUNT * HEAD, D), 0.15, 0.8984375, ((1, 32), (2, 8)))
    return {"tokens": tokens, "norm_gain": norm_gain, "qk_gain": qk_gain, "w_query_window": w_query_window, "w_key_window": w_key_window, "w_value_window": w_value_window, "sink_logits": sink_logits, "w_query_forget": w_query_forget, "w_key_forget": w_key_forget, "w_value_forget": w_value_forget, "gate_cum": gate_cum, "w_merge": w_merge, "w_branch": w_branch}


epsilon = 1e-06
big_negative = -1e+30

def rounded(value):
    return lax.optimization_barrier(value.astype(jnp.bfloat16)).astype(jnp.float32)

def head_norm(raw, gain, head_count):
    split = raw.reshape(raw.shape[0], head_count, -1)
    scaled = split * lax.rsqrt(lax.optimization_barrier(jnp.mean(split * split, axis=-1, keepdims=True)) + epsilon) * gain
    return scaled.astype(jnp.bfloat16)

def window_attend(queries, keys_ext, values_ext, sink_rows, first_pos):
    row_count, head_count, head_size = queries.shape
    group_count = keys_ext.shape[1]
    span_rows = WINDOW // 2
    block_count = row_count // span_rows
    query_blocks = queries.reshape(block_count, span_rows, group_count, head_count // group_count, head_size).astype(jnp.float32)
    key_blocks = jnp.concatenate([keys_ext[lag_index * span_rows:lag_index * span_rows + row_count].reshape(block_count, span_rows, group_count, head_size) for lag_index in range(3)], axis=1).astype(jnp.float32)
    value_blocks = jnp.concatenate([values_ext[lag_index * span_rows:lag_index * span_rows + row_count].reshape(block_count, span_rows, group_count, head_size) for lag_index in range(3)], axis=1).astype(jnp.float32)
    scores = jnp.einsum('nqgrd,nkgd->ngrqk', query_blocks, key_blocks) * head_size ** (-0.5)
    distance = WINDOW + jnp.arange(span_rows)[:, None] - jnp.arange(3 * span_rows)[None, :]
    key_pos = first_pos - WINDOW + jnp.arange(block_count)[:, None] * span_rows + jnp.arange(3 * span_rows)[None, :]
    is_valid = ((distance >= 0) & (distance < WINDOW))[None] & (key_pos >= 0)[:, None, :]
    is_valid = is_valid[:, None, None]
    sink_grid = sink_rows.reshape(1, group_count, head_count // group_count, 1)
    row_max = jnp.maximum(lax.optimization_barrier(jnp.max(jnp.where(is_valid, scores, big_negative), axis=-1)), sink_grid)
    weights = jnp.where(is_valid, jnp.exp(scores - row_max[..., None]), 0.0)
    row_total = lax.optimization_barrier(jnp.sum(weights, axis=-1)) + jnp.exp(sink_grid - row_max)
    prob_rows = rounded(weights / row_total[..., None])
    mixed_sum = jnp.einsum('ngrqk,nkgd->nqgrd', prob_rows, value_blocks)
    return mixed_sum.reshape(row_count, head_count * head_size).astype(jnp.bfloat16)

def forget_attend(queries, keys, values, gates):
    row_count, head_count, head_size = queries.shape
    block_rows = math.gcd(row_count, 512)
    block_count = row_count // block_rows
    key_float = keys.astype(jnp.float32)
    value_float = values.astype(jnp.float32)
    key_pos = jnp.arange(row_count)

    def one_block(inputs):
        block_index, query_block, gate_block = inputs
        scores = jnp.einsum('qhd,khd->hqk', query_block.astype(jnp.float32), key_float) * head_size ** (-0.5)
        scores = scores + gate_block.T[:, :, None] - gates.T[:, None, :]
        query_pos = block_index * block_rows + jnp.arange(block_rows)
        is_valid = (query_pos[:, None] >= key_pos[None, :])[None]
        scores = jnp.where(is_valid, scores, big_negative)
        row_max = lax.optimization_barrier(jnp.max(scores, axis=-1))
        weights = jnp.where(is_valid, jnp.exp(scores - row_max[..., None]), 0.0)
        row_total = lax.optimization_barrier(jnp.sum(weights, axis=-1))
        mixed_sum = jnp.einsum('hqk,khd->qhd', rounded(weights), value_float)
        return mixed_sum / row_total.T[:, :, None]
    result = lax.map(one_block, (jnp.arange(block_count), queries.reshape(block_count, block_rows, head_count, head_size), gates.reshape(block_count, block_rows, head_count)))
    return result.reshape(row_count, head_count * head_size).astype(jnp.bfloat16)

def reference(tokens, norm_gain, qk_gain, w_query_window, w_key_window, w_value_window, sink_logits, w_query_forget, w_key_forget, w_value_forget, gate_cum, w_merge, w_branch):
    as_float = tokens.astype(jnp.float32)
    normed = (as_float * lax.rsqrt(lax.optimization_barrier(jnp.mean(as_float * as_float, axis=-1, keepdims=True)) + epsilon) * norm_gain).astype(jnp.bfloat16)

    def project(weight):
        return jnp.dot(normed, weight, preferred_element_type=jnp.float32)
    window_query = head_norm(project(w_query_window), qk_gain[0], QUERY_HEAD_COUNT)
    window_key = head_norm(project(w_key_window), qk_gain[1], KV_HEADS)
    window_value = project(w_value_window).astype(jnp.bfloat16).reshape(SEQUENCE_LENGTH, KV_HEADS, HEAD)
    padding = jnp.zeros((WINDOW, KV_HEADS, HEAD), jnp.bfloat16)
    window_out = window_attend(window_query, jnp.concatenate([padding, window_key], axis=0), jnp.concatenate([padding, window_value], axis=0), sink_logits, 0)
    forget_query = head_norm(project(w_query_forget), qk_gain[2], QUERY_HEAD_COUNT)
    forget_key = head_norm(project(w_key_forget), qk_gain[3], QUERY_HEAD_COUNT)
    forget_value = project(w_value_forget).astype(jnp.bfloat16).reshape(SEQUENCE_LENGTH, QUERY_HEAD_COUNT, HEAD)
    forget_out = forget_attend(forget_query, forget_key, forget_value, gate_cum)
    merge_gate = jax.nn.sigmoid(project(w_merge.reshape(D, 2 * D))).reshape(SEQUENCE_LENGTH, 2, D)
    window_projection = jnp.dot(window_out, w_branch[0], preferred_element_type=jnp.float32)
    forget_projection = jnp.dot(forget_out, w_branch[1], preferred_element_type=jnp.float32)
    return (merge_gate[:, 0] * window_projection + merge_gate[:, 1] * forget_projection).astype(jnp.bfloat16)
```

```python
import functools
import math

import jax
import jax.numpy as jnp
from jax import lax
from jax.experimental import pallas as pl
from jax.experimental.pallas import tpu as pltpu
from jax.sharding import PartitionSpec as P

HEAD = 64
PAIR = 2 * HEAD
WINDOW = 128
MESH = pl.DeviceIdType.MESH

epsilon = 1e-06
big_negative = -1e30
log2e = math.log2(math.e)


def low_half(shape):
    return lax.broadcasted_iota(jnp.int32, shape, 1) < HEAD


def pair_norm(raw, gain):
    low = low_half(raw.shape)
    squares = raw * raw
    first = jnp.sum(jnp.where(low, squares, 0.0), axis=1, keepdims=True)
    second = jnp.sum(jnp.where(low, 0.0, squares), axis=1, keepdims=True)
    mean = jnp.where(low, first, second) * (1.0 / HEAD)
    return raw * lax.rsqrt(mean + epsilon) * gain


def dot_nt(a, b):
    return lax.dot_general(a, b, (((1,), (1,)), ((), ())), preferred_element_type=jnp.float32)


class TpGather:
    def __init__(self, source, buf, t, chips, sems):
        self.source, self.buf, self.chips = source, buf, chips
        self.send, self.recv, self.relay_send, self.relay_recv = sems
        self.t, self.x, self.core = t, t // 2, t % 2
        self.steps = chips // 2
        self.half = buf.shape[1] // 2

    def slot(self, x, core):
        return lax.rem(x + 2 * self.chips, self.chips) * 2 + core

    def block(self, d, s):
        return self.slot(self.x - s if d == 0 else self.x + s, self.core)

    def parts(self, d, s):
        return (0, 1) if s < self.steps - 1 else (d,)

    def ring(self, d, s, c):
        block = self.block(d, s)
        rows = pl.ds(c * self.half, self.half)
        dst = self.buf.at[block, rows]
        src = self.source.at[rows] if s == 0 and self.source is not None else dst
        peer = self.slot(self.x + (1 if d == 0 else -1), self.core)
        return pltpu.make_async_remote_copy(
            src_ref=src,
            dst_ref=dst,
            send_sem=self.send.at[d, s, c],
            recv_sem=self.recv.at[d, s, c],
            device_id={"tp": peer},
            device_id_type=MESH,
        )

    def relay(self, k, block):
        dst = self.buf.at[block]
        src = self.source if k == 0 and self.source is not None else dst
        return pltpu.make_async_remote_copy(
            src_ref=src,
            dst_ref=dst,
            send_sem=self.relay_send.at[k],
            recv_sem=self.relay_recv.at[k],
            device_id={"tp": self.t + 1 - 2 * self.core},
            device_id_type=MESH,
        )

    def relays(self):
        order = [(0, 0)]
        for s in range(self.steps - 1):
            order += [(1 + 2 * s, -(s + 1)), (2 + 2 * s, s + 1)]
        return order + [(self.chips - 1, self.steps)]

    def begin(self):
        for d in (0, 1):
            for c in self.parts(d, 0):
                self.ring(d, 0, c).start()
        self.relay(0, self.slot(self.x, self.core)).start()

    def advance(self, s):
        for d in (0, 1):
            for c in self.parts(d, s):
                self.ring(d, s, c).wait_recv()
                if s + 1 < self.steps and c in self.parts(d, s + 1):
                    self.ring(d, s + 1, c).start()
        if s + 1 < self.steps:
            self.relay(1 + 2 * s, self.slot(self.x - s - 1, self.core)).start()
            self.relay(2 + 2 * s, self.slot(self.x + s + 1, self.core)).start()
        else:
            self.relay(self.chips - 1, self.slot(self.x + self.steps, self.core)).start()

    def finish(self):
        for k, offset in self.relays():
            self.relay(k, self.slot(self.x + offset, 1 - self.core)).wait_recv()

    def drain(self):
        for d in (0, 1):
            for s in range(self.steps):
                for c in self.parts(d, s):
                    self.ring(d, s, c).wait_send()
        for k, offset in self.relays():
            self.relay(k, self.slot(self.x + offset, self.core)).wait_send()


def kernel(
    n,
    tp,
    tok_ref,
    w_ref,
    gate_ref,
    gain_ref,
    qk_gain_ref,
    sink_ref,
    out_ref,
    tokb,
    nb,
    wb,
    gb,
    kv,
    prev,
    keys_ext,
    values_ext,
    wqb,
    fqb,
    fob,
    wob,
    sgb,
    mixb,
    accb,
    maxb,
    sumb,
    w_send,
    w_recv,
    g_send,
    g_recv,
    kv_send,
    kv_recv,
    prev_send,
    prev_recv,
    *tp_sems,
):
    me = lax.axis_index("sp")
    t = lax.axis_index("tp")
    right, left = lax.rem(me + 1, n), lax.rem(me + n - 1, n)
    chips = tp // 2
    rows, cols = tok_ref.shape
    depth = w_ref.shape[0]
    width = gain_ref.shape[1]
    w_parts = w_recv.shape[2]
    w_rows = depth // w_parts
    last = n // 2 - 1
    tiles = rows // 128
    first_branch = w_ref.shape[1] - cols
    first_merge = first_branch - 2 * cols

    tokens = TpGather(tok_ref, tokb, t, chips, tp_sems[0:4])
    window_outs = TpGather(None, wob, t, chips, tp_sems[4:8])
    forget_outs = TpGather(None, fob, t, chips, tp_sems[8:12])

    barrier = pltpu.get_barrier_semaphore()
    greeted = [
        {"sp": right},
        {"sp": left},
        {"tp": tokens.slot(tokens.x + 1, tokens.core)},
        {"tp": tokens.slot(tokens.x - 1, tokens.core)},
        {"tp": t + 1 - 2 * tokens.core},
    ]
    for device in greeted:
        pl.semaphore_signal(barrier, inc=1, device_id=device, device_id_type=MESH)
    pl.semaphore_wait(barrier, len(greeted))

    def ring_block(d, s):
        return lax.rem(me + n - s, n) if d == 0 else lax.rem(me + s, n)

    def to_next(d):
        return {"sp": right if d == 0 else left}

    def ring_copy(src, dst, send, recv, d):
        return pltpu.make_async_remote_copy(
            src_ref=src,
            dst_ref=dst,
            send_sem=send,
            recv_sem=recv,
            device_id=to_next(d),
            device_id_type=MESH,
        )

    def w_copy(d, s, q, own=False):
        part = pl.ds(q * w_rows, w_rows)
        dst = wb.at[ring_block(d, s), part]
        return ring_copy(w_ref.at[part] if own else dst, dst, w_send.at[d, s, q], w_recv.at[d, s, q], d)

    def g_copy(d, s, own=False):
        dst = gb.at[ring_block(d, s)]
        return ring_copy(gate_ref if own else dst, dst, g_send.at[d, s], g_recv.at[d, s], d)

    kv_parts = kv_recv.shape[2]
    kv_rows = rows // kv_parts

    def kv_copy(d, s, q):
        dst = kv.at[ring_block(d, s), pl.ds(q * kv_rows, kv_rows)]
        return ring_copy(dst, dst, kv_send.at[d, s, q], kv_recv.at[d, s, q], d)

    for d in (0, 1):
        if d == 0 or last > 0:
            g_copy(d, 0, own=True).start()
            for q in range(w_parts):
                w_copy(d, 0, q, own=True).start()
    wb[me] = w_ref[...]
    gb[me] = gate_ref[...]
    tokb[t] = tok_ref[...]

    def normalize():
        tokens.finish()
        for r in range(tiles):
            part = pl.ds(r * 128, 128)
            total = jnp.zeros((128, 1), jnp.float32)
            for k in range(tp):
                x = tokb[k, part].astype(jnp.float32)
                total += jnp.sum(x * x, axis=1, keepdims=True)
            scale = lax.rsqrt(total * (1.0 / width) + epsilon)
            for k in range(tp):
                x = tokb[k, part].astype(jnp.float32)
                nb[part, k * cols : (k + 1) * cols] = (
                    x * scale * gain_ref[:, k * cols : (k + 1) * cols]
                ).astype(jnp.bfloat16)

    def run_at(step, tasks, spacing):
        for k, task in enumerate(tasks):
            at = 1 + k * spacing
            if at <= last:
                pl.when(step == at)(task)

    def run_late(tasks, spacing):
        for k, task in enumerate(tasks):
            if 1 + k * spacing > last:
                task()

    token_tasks = [functools.partial(tokens.advance, s) for s in range(tokens.steps)] + [normalize]
    tokens.begin()

    def w_step(s, carry):
        for q in range(w_parts):
            for d in (0, 1):
                w_copy(d, s - 1, q).wait_recv()
                if d == 0:
                    w_copy(d, s, q).start()
                else:
                    pl.when(s < last)(w_copy(d, s, q).start)
        for d in (0, 1):
            g_copy(d, s - 1).wait_recv()
            if d == 0:
                g_copy(d, s).start()
            else:
                pl.when(s < last)(g_copy(d, s).start)
        run_at(s, token_tasks, 2)
        return carry

    lax.fori_loop(1, last + 1, w_step, 0)
    run_late(token_tasks, 2)
    g_copy(0, last).wait_recv()
    for q in range(w_parts):
        w_copy(0, last, q).wait_recv()

    def project(start, size):
        weights = wb[:, :, start : start + size].reshape(width, size)
        return jnp.dot(nb[...], weights, preferred_element_type=jnp.float32)

    both = project(0, 2 * PAIR)
    kv[me, :, 0:PAIR] = pair_norm(both[:, 0:PAIR], qk_gain_ref[3:4, :]).astype(jnp.bfloat16)
    kv[me, :, PAIR : 2 * PAIR] = both[:, PAIR : 2 * PAIR].astype(jnp.bfloat16)

    def split_heads(dst, query):
        low = low_half(query.shape)
        dst[0] = jnp.where(low, query, 0.0).astype(jnp.bfloat16)
        dst[1] = jnp.where(low, 0.0, query).astype(jnp.bfloat16)

    both = project(2 * PAIR, 2 * PAIR)
    for d in (0, 1):
        for q in range(kv_parts):
            if last > 0 or q == d:
                kv_copy(d, 0, q).start()
    split_heads(fqb, pair_norm(both[:, 0:PAIR], qk_gain_ref[2:3, :]))
    split_heads(wqb, pair_norm(both[:, PAIR : 2 * PAIR], qk_gain_ref[0:1, :]))

    to_log2 = log2e * HEAD ** (-0.5)

    def absorb(block, own):
        for h in (0, 1):
            key_gate = (gb[me, h : h + 1, 0:1] - gb[block, h : h + 1, :]) * log2e
            for r in range(tiles):
                part = pl.ds(r * 128, 128)
                span = (r + 1) * 128 if own else rows
                scores = dot_nt(fqb[h, part], kv[block, 0:span, 0:PAIR]) * to_log2 + key_gate[:, 0:span]
                if own:
                    query_pos = r * 128 + lax.broadcasted_iota(jnp.int32, scores.shape, 0)
                    key_pos = lax.broadcasted_iota(jnp.int32, scores.shape, 1)
                    scores = jnp.where(query_pos >= key_pos, scores, big_negative)
                top = jnp.max(scores, axis=1, keepdims=True)
                if not own:
                    before = maxb[h, part]
                    top = jnp.maximum(before, top)
                weights = jnp.exp2(scores - top)
                partial = weights[:, 0:128]
                for k in range(1, span // 128):
                    partial += weights[:, k * 128 : (k + 1) * 128]
                product = jnp.dot(
                    weights.astype(jnp.bfloat16),
                    kv[block, 0:span, PAIR : 2 * PAIR],
                    preferred_element_type=jnp.float32,
                )
                if not own:
                    shrink = jnp.exp2(before - top)
                    partial += sumb[h, part] * shrink
                    product += accb[h, part] * shrink
                maxb[h, part] = top
                sumb[h, part] = partial
                accb[h, part] = product

    def window_project():
        raw = project(4 * PAIR, PAIR)
        low = low_half(raw.shape)
        mean = jnp.sum(jnp.where(low, raw * raw, 0.0), axis=1, keepdims=True) * (1.0 / HEAD)
        key = raw * lax.rsqrt(mean + epsilon) * qk_gain_ref[1:2, :]
        ext = jnp.where(low, key, raw)
        turned = pltpu.roll(ext, HEAD, 1)
        keys_ext[WINDOW:, :] = jnp.where(low, ext, turned).astype(jnp.bfloat16)
        values_ext[WINDOW:, :] = jnp.where(low, turned, ext).astype(jnp.bfloat16)
        prev[0] = ext[rows - WINDOW :, :].astype(jnp.bfloat16)

    def prev_copy():
        return ring_copy(prev.at[0], prev.at[1], prev_send, prev_recv, 0)

    def window_send():
        prev_copy().start()

    def window_attend():
        prev_copy().wait_recv()
        ext = prev[1].astype(jnp.float32)
        low = low_half(ext.shape)
        turned = pltpu.roll(ext, HEAD, 1)
        keys_ext[0:WINDOW, :] = jnp.where(low, ext, turned).astype(jnp.bfloat16)
        values_ext[0:WINDOW, :] = jnp.where(low, turned, ext).astype(jnp.bfloat16)
        for r in range(tiles):
            part = pl.ds(r * 128, 128)
            outs = []
            for h in (0, 1):
                span = pl.ds(r * 128, 128 + WINDOW)
                scores = dot_nt(wqb[h, part], keys_ext[span, :]) * HEAD ** (-0.5)
                distance = (
                    WINDOW
                    + lax.broadcasted_iota(jnp.int32, scores.shape, 0)
                    - lax.broadcasted_iota(jnp.int32, scores.shape, 1)
                )
                key_pos = (
                    me * rows + r * 128 - WINDOW + lax.broadcasted_iota(jnp.int32, scores.shape, 1)
                )
                valid = (distance >= 0) & (distance < WINDOW) & (key_pos >= 0)
                sink = sink_ref[h]
                top = jnp.maximum(
                    jnp.max(jnp.where(valid, scores, big_negative), axis=1, keepdims=True), sink
                )
                weights = jnp.where(valid, jnp.exp(scores - top), 0.0)
                total = jnp.sum(weights, axis=1, keepdims=True) + jnp.exp(sink - top)
                probs = (weights / total).astype(jnp.bfloat16)
                outs.append(
                    jnp.dot(probs, values_ext[span, :], preferred_element_type=jnp.float32)
                )
            merged = jnp.where(low_half(outs[0].shape), outs[0], outs[1])
            wob[t, part] = merged.astype(jnp.bfloat16)

    def merge_project(b):
        logits = project(first_merge + b * cols, cols)
        sgb[b] = jax.nn.sigmoid(logits)

    def branch_project(buf, b):
        per = n // tp
        high = depth // 2
        total = jnp.zeros((rows, cols), jnp.float32)
        for k in range(tp):
            weights = wb[k * per : (k + 1) * per, b * high : (b + 1) * high, first_branch:].reshape(
                per * high, cols
            )
            total += jnp.dot(buf[k], weights, preferred_element_type=jnp.float32)
        return total

    def window_mix():
        window_outs.finish()
        mixb[...] = sgb[0] * branch_project(wob, 0)

    absorb(me, True)
    tasks = (
        [window_project, window_send, window_attend, window_outs.begin]
        + [functools.partial(window_outs.advance, s) for s in range(window_outs.steps)]
        + [functools.partial(merge_project, b) for b in (0, 1)]
        + [window_mix]
    )

    def kv_step(s, carry):
        for q in range(kv_parts):
            for d in (0, 1):
                kv_copy(d, s - 1, q).wait_recv()
                if q == d:
                    kv_copy(d, s, q).start()
                else:
                    pl.when(s < last)(kv_copy(d, s, q).start)
        run_at(s, tasks, 1)
        pl.when(me >= s)(functools.partial(absorb, lax.rem(me + n - s, n), False))
        pl.when(me + s >= n)(functools.partial(absorb, lax.rem(me + s, n), False))
        return carry

    lax.fori_loop(1, last + 1, kv_step, 0)
    run_late(tasks, 1)
    kv_copy(0, last, 0).wait_recv()
    kv_copy(1, last, 1).wait_recv()
    pl.when(me >= n // 2)(functools.partial(absorb, lax.rem(me + n // 2, n), False))

    for r in range(tiles):
        part = pl.ds(r * 128, 128)
        outs = [accb[h, part] / jnp.sum(sumb[h, part], axis=1, keepdims=True) for h in (0, 1)]
        merged = jnp.where(low_half(outs[0].shape), outs[0], outs[1])
        fob[t, part] = merged.astype(jnp.bfloat16)
    forget_outs.begin()
    for s in range(forget_outs.steps):
        forget_outs.advance(s)
    forget_outs.finish()
    out_ref[...] = (mixb[...] + sgb[1] * branch_project(fob, 1)).astype(jnp.bfloat16)

    def drain_step(s, carry):
        for d in (0, 1):

            def full(d=d):
                g_copy(d, s).wait_send()
                for q in range(w_parts):
                    w_copy(d, s, q).wait_send()

            if d == 0:
                full()
            else:
                pl.when(s < last)(full)
            for q in range(kv_parts):
                if q == d:
                    kv_copy(d, s, q).wait_send()
                else:
                    pl.when(s < last)(kv_copy(d, s, q).wait_send)
        return carry

    lax.fori_loop(0, last + 1, drain_step, 0)
    prev_copy().wait_send()
    for gather in (tokens, window_outs, forget_outs):
        gather.drain()


def on_device(
    n,
    tp,
    tokens,
    norm_gain,
    qk_gain,
    w_query_window,
    w_key_window,
    w_value_window,
    sink_logits,
    w_query_forget,
    w_key_forget,
    w_value_forget,
    gate_cum,
    w_merge,
    w_branch,
):
    rows, cols = tokens.shape
    depth = w_merge.shape[0]
    width = norm_gain.shape[0]
    weights = jnp.concatenate(
        [
            w_key_forget,
            w_value_forget,
            w_query_forget,
            w_query_window,
            w_key_window,
            w_value_window,
            w_merge.reshape(depth, -1),
            w_branch.reshape(depth, -1),
        ],
        axis=1,
    )
    steps, chips = n // 2, tp // 2
    tp_sems = [
        pltpu.SemaphoreType.DMA((2, max(chips // 2, 1), 2)),
        pltpu.SemaphoreType.DMA((2, max(chips // 2, 1), 2)),
        pltpu.SemaphoreType.DMA((chips,)),
        pltpu.SemaphoreType.DMA((chips,)),
    ]
    w_parts, kv_parts = 2, 2
    bf16, f32 = jnp.bfloat16, jnp.float32
    vmem = pl.BlockSpec(memory_space=pltpu.VMEM)
    return pl.pallas_call(
        functools.partial(kernel, n, tp),
        out_shape=jax.ShapeDtypeStruct((rows, cols), bf16),
        in_specs=[vmem] * 5 + [pl.BlockSpec(memory_space=pltpu.SMEM)],
        out_specs=vmem,
        scratch_shapes=[
            pltpu.VMEM((tp, rows, cols), bf16),
            pltpu.VMEM((rows, width), bf16),
            pltpu.VMEM((n, depth, weights.shape[1]), bf16),
            pltpu.VMEM((n, 2, rows), f32),
            pltpu.VMEM((n, rows, 2 * PAIR), bf16),
            pltpu.VMEM((2, WINDOW, PAIR), bf16),
            pltpu.VMEM((WINDOW + rows, PAIR), bf16),
            pltpu.VMEM((WINDOW + rows, PAIR), bf16),
            pltpu.VMEM((2, rows, PAIR), bf16),
            pltpu.VMEM((2, rows, PAIR), bf16),
            pltpu.VMEM((tp, rows, PAIR), bf16),
            pltpu.VMEM((tp, rows, PAIR), bf16),
            pltpu.VMEM((2, rows, cols), f32),
            pltpu.VMEM((rows, cols), f32),
            pltpu.VMEM((2, rows, PAIR), f32),
            pltpu.VMEM((2, rows, 1), f32),
            pltpu.VMEM((2, rows, PAIR), f32),
            pltpu.SemaphoreType.DMA((2, steps, w_parts)),
            pltpu.SemaphoreType.DMA((2, steps, w_parts)),
            pltpu.SemaphoreType.DMA((2, steps)),
            pltpu.SemaphoreType.DMA((2, steps)),
            pltpu.SemaphoreType.DMA((2, steps, kv_parts)),
            pltpu.SemaphoreType.DMA((2, steps, kv_parts)),
            pltpu.SemaphoreType.DMA,
            pltpu.SemaphoreType.DMA,
        ]
        + tp_sems * 3,
        compiler_params=pltpu.CompilerParams(
            collective_id=0, has_side_effects=True, vmem_limit_bytes=60 * 1024 * 1024
        ),
    )(
        tokens,
        weights,
        gate_cum.T,
        norm_gain.reshape(1, width),
        jnp.concatenate([qk_gain, qk_gain], axis=1),
        sink_logits,
    )


def solution(mesh):
    return jax.shard_map(
        functools.partial(on_device, mesh.shape["sp"], mesh.shape["tp"]),
        mesh=mesh,
        in_specs=(
            P(("grp", "sp"), "tp"),
            P(),
            P(),
            P("sp", "tp"),
            P("sp", "tp"),
            P("sp", "tp"),
            P("tp"),
            P("sp", "tp"),
            P("sp", "tp"),
            P("sp", "tp"),
            P(("grp", "sp"), "tp"),
            P("sp", None, "tp"),
            P(None, "sp", "tp"),
        ),
        out_specs=P(("grp", "sp"), "tp"),
        check_vma=False,
    )
```

```python
import functools
import math

import jax
import jax.numpy as jnp
from jax import lax
from jax.experimental import pallas as pl
from jax.experimental.pallas import tpu as pltpu
from jax.sharding import PartitionSpec as P

HEAD = 64
PAIR = 2 * HEAD
WINDOW = 128
MESH = pl.DeviceIdType.MESH

epsilon = 1e-06
big_negative = -1e30
log2e = math.log2(math.e)


def low_half(shape):
    return lax.broadcasted_iota(jnp.int32, shape, 1) < HEAD


def pair_norm(raw, gain):
    low = low_half(raw.shape)
    squares = raw * raw
    first = jnp.sum(jnp.where(low, squares, 0.0), axis=1, keepdims=True)
    second = jnp.sum(jnp.where(low, 0.0, squares), axis=1, keepdims=True)
    mean = jnp.where(low, first, second) * (1.0 / HEAD)
    return raw * lax.rsqrt(mean + epsilon) * gain


def dot_nt(a, b):
    return lax.dot_general(a, b, (((1,), (1,)), ((), ())), preferred_element_type=jnp.float32)


class TpGather:
    def __init__(self, source, buf, t, chips, sems):
        self.source, self.buf, self.chips = source, buf, chips
        self.send, self.recv, self.relay_send, self.relay_recv = sems
        self.t, self.x, self.core = t, t // 2, t % 2
        self.steps = chips // 2
        self.half = buf.shape[1] // 2

    def slot(self, x, core):
        return lax.rem(x + 2 * self.chips, self.chips) * 2 + core

    def block(self, d, s):
        return self.slot(self.x - s if d == 0 else self.x + s, self.core)

    def parts(self, d, s):
        return (d, 1 - d) if s < self.steps - 1 else (d,)

    def ring(self, d, s, c):
        block = self.block(d, s)
        rows = pl.ds(c * self.half, self.half)
        dst = self.buf.at[block, rows]
        src = self.source.at[rows] if s == 0 and self.source is not None else dst
        peer = self.slot(self.x + (1 if d == 0 else -1), self.core)
        return pltpu.make_async_remote_copy(
            src_ref=src,
            dst_ref=dst,
            send_sem=self.send.at[d, s, c],
            recv_sem=self.recv.at[d, s, c],
            device_id={"tp": peer},
            device_id_type=MESH,
        )

    def relay(self, k, block):
        dst = self.buf.at[block]
        src = self.source if k == 0 and self.source is not None else dst
        return pltpu.make_async_remote_copy(
            src_ref=src,
            dst_ref=dst,
            send_sem=self.relay_send.at[k],
            recv_sem=self.relay_recv.at[k],
            device_id={"tp": self.t + 1 - 2 * self.core},
            device_id_type=MESH,
        )

    def relays(self):
        order = [(0, 0)]
        for s in range(self.steps - 1):
            order += [(1 + 2 * s, -(s + 1)), (2 + 2 * s, s + 1)]
        return order + [(self.chips - 1, self.steps)]

    def begin(self):
        for d in (0, 1):
            for c in self.parts(d, 0):
                self.ring(d, 0, c).start()
        self.relay(0, self.slot(self.x, self.core)).start()

    def advance(self, s):
        for k in range(len(self.parts(0, s))):
            for d in (0, 1):
                c = self.parts(d, s)[k]
                self.ring(d, s, c).wait_recv()
                if s + 1 < self.steps and c in self.parts(d, s + 1):
                    self.ring(d, s + 1, c).start()
        if s + 1 < self.steps:
            self.relay(1 + 2 * s, self.slot(self.x - s - 1, self.core)).start()
            self.relay(2 + 2 * s, self.slot(self.x + s + 1, self.core)).start()
        else:
            self.relay(self.chips - 1, self.slot(self.x + self.steps, self.core)).start()

    def finish(self):
        for k, offset in self.relays():
            self.relay(k, self.slot(self.x + offset, 1 - self.core)).wait_recv()

    def drain(self):
        for d in (0, 1):
            for s in range(self.steps):
                for c in self.parts(d, s):
                    self.ring(d, s, c).wait_send()
        for k, offset in self.relays():
            self.relay(k, self.slot(self.x + offset, self.core)).wait_send()


def kernel(
    n,
    tp,
    share,
    tok_ref,
    w_ref,
    gate_ref,
    gain_ref,
    qk_gain_ref,
    sink_ref,
    out_ref,
    tokb,
    nb,
    wb,
    gb,
    gates,
    kb,
    vb,
    prev,
    keys_ext,
    values_ext,
    wqb,
    fqb,
    fob,
    wob,
    sgb,
    mixb,
    accb,
    maxb,
    sumb,
    w_send,
    w_recv,
    pair_send,
    pair_recv,
    g_send,
    g_recv,
    kv_send,
    kv_recv,
    prev_send,
    prev_recv,
    *tp_sems,
):
    me = lax.axis_index("sp")
    t = lax.axis_index("tp")
    right, left = lax.rem(me + 1, n), lax.rem(me + n - 1, n)
    chips = tp // 2
    rows, cols = tok_ref.shape
    depth = w_ref.shape[0]
    width = gain_ref.shape[1]
    quarter = depth // 4
    group = lax.axis_index("grp")
    odd = group % 2
    quarters = [2 + odd, 0, 1] if share else [0, 1, 2, 3]
    cuts = [0, w_ref.shape[1] - 3 * tok_ref.shape[1], w_ref.shape[1]]
    last = n // 2 - 1
    tiles = rows // 128
    first_branch = w_ref.shape[1] - cols
    first_merge = first_branch - 2 * cols

    tokens = TpGather(tok_ref, tokb, t, chips, tp_sems[0:4])
    window_outs = TpGather(None, wob, t, chips, tp_sems[4:8])
    forget_outs = TpGather(None, fob, t, chips, tp_sems[8:12])

    barrier = pltpu.get_barrier_semaphore()
    greeted = [
        {"sp": right},
        {"sp": left},
        {"tp": tokens.slot(tokens.x + 1, tokens.core)},
        {"tp": tokens.slot(tokens.x - 1, tokens.core)},
        {"tp": t + 1 - 2 * tokens.core},
    ]
    if share:
        greeted.append({"grp": group + 1 - 2 * odd})
    for device in greeted:
        pl.semaphore_signal(barrier, inc=1, device_id=device, device_id_type=MESH)
    pl.semaphore_wait(barrier, len(greeted))

    def ring_block(d, s):
        return lax.rem(me + n - s, n) if d == 0 else lax.rem(me + s, n)

    def to_next(d):
        return {"sp": right if d == 0 else left}

    def ring_copy(src, dst, send, recv, d):
        return pltpu.make_async_remote_copy(
            src_ref=src,
            dst_ref=dst,
            send_sem=send,
            recv_sem=recv,
            device_id=to_next(d),
            device_id_type=MESH,
        )

    def quarter_rows(k):
        return pl.ds(k * quarter if isinstance(k, int) else pl.multiple_of(k * quarter, 16), quarter)

    def w_copy(d, s, q, c, own=False):
        rows_of, cols_of = quarter_rows(quarters[q]), pl.ds(cuts[c], cuts[c + 1] - cuts[c])
        dst = wb.at[ring_block(d, s), rows_of, cols_of]
        src = w_ref.at[rows_of, cols_of] if own else dst
        k = 2 * q + c
        return ring_copy(src, dst, w_send.at[d, s, k], w_recv.at[d, s, k], d)

    def pair_copy(d, s):
        block = wb.at[ring_block(d, s + 1), quarter_rows(quarters[0])]
        return pltpu.make_async_remote_copy(
            src_ref=block,
            dst_ref=block,
            send_sem=pair_send.at[d, s],
            recv_sem=pair_recv.at[d, s],
            device_id={"grp": group + 1 - 2 * odd},
            device_id_type=MESH,
        )

    def g_copy(d, s, own=False):
        dst = gb.at[ring_block(d, s)]
        return ring_copy(gate_ref if own else dst, dst, g_send.at[d, s], g_recv.at[d, s], d)

    kv_parts = 4

    def kv_copy(d, s, q):
        block = ring_block(d, s)
        if q % 2 == 0:
            dst = kb.at[block, pl.ds(q // 2 * (rows // 2), rows // 2)]
        else:
            dst = vb.at[block, pl.ds(q // 2 * HEAD, HEAD)]
        return ring_copy(dst, dst, kv_send.at[d, s, q], kv_recv.at[d, s, q], d)

    def halfway(d, q):
        return q // 2 == d

    for d in (0, 1):
        if d == 0 or last > 0:
            g_copy(d, 0, own=True).start()
    for q in range(len(quarters)):
        for c in (0, 1):
            for d in (0, 1):
                if d == 0 or last > 0:
                    w_copy(d, 0, q, c, own=True).start()
    wb[me] = w_ref[...]
    gb[me] = gate_ref[...]
    tokb[t] = tok_ref[...]

    def normalize():
        tokens.finish()
        for r in range(tiles):
            part = pl.ds(r * 128, 128)
            total = jnp.zeros((128, 1), jnp.float32)
            for k in range(tp):
                x = tokb[k, part].astype(jnp.float32)
                total += jnp.sum(x * x, axis=1, keepdims=True)
            scale = lax.rsqrt(total * (1.0 / width) + epsilon)
            for k in range(tp):
                x = tokb[k, part].astype(jnp.float32)
                nb[part, k * cols : (k + 1) * cols] = (
                    x * scale * gain_ref[:, k * cols : (k + 1) * cols]
                ).astype(jnp.bfloat16)

    def run_at(step, tasks, spacing):
        for k, task in enumerate(tasks):
            at = 1 + k * spacing
            if at <= last:
                pl.when(step == at)(task)

    def run_late(tasks, spacing):
        for k, task in enumerate(tasks):
            if 1 + k * spacing > last:
                task()

    token_tasks = [functools.partial(tokens.advance, s) for s in range(tokens.steps)] + [normalize]
    tokens.begin()

    def turn_gates(block):
        pair = gb[block]
        gates[block, :, 0:8] = jnp.transpose(jnp.concatenate([pair] * 4, axis=0)) * log2e

    def w_step(s, carry):
        for q in range(len(quarters)):
            for c in (0, 1):
                for d in (0, 1):
                    w_copy(d, s - 1, q, c).wait_recv()
                    if d == 0:
                        w_copy(d, s, q, c).start()
                    else:
                        pl.when(s < last)(w_copy(d, s, q, c).start)
            if share and q == 0:
                for d in (0, 1):
                    pair_copy(d, s - 1).start()
        for d in (0, 1):
            g_copy(d, s - 1).wait_recv()
            if d == 0:
                g_copy(d, s).start()
            else:
                pl.when(s < last)(g_copy(d, s).start)
        turn_gates(ring_block(0, s))
        turn_gates(ring_block(1, s))
        run_at(s, token_tasks, 2)
        return carry

    lax.fori_loop(1, last + 1, w_step, 0)
    run_late(token_tasks, 2)
    for q in range(len(quarters)):
        for c in (0, 1):
            w_copy(0, last, q, c).wait_recv()
        if share and q == 0:
            pair_copy(0, last).start()
    g_copy(0, last).wait_recv()
    turn_gates(ring_block(0, last + 1))
    turn_gates(me)
    if share:

        def pair_step(s, carry):
            pair_copy(0, s).wait_recv()
            pl.when(s < last)(pair_copy(1, s).wait_recv)
            return carry

        lax.fori_loop(0, last + 1, pair_step, 0)

    def project(start, size):
        weights = wb[:, :, start : start + size].reshape(width, size)
        return jnp.dot(nb[...], weights, preferred_element_type=jnp.float32)

    both = project(0, 2 * PAIR)
    kb[me] = pair_norm(both[:, 0:PAIR], qk_gain_ref[3:4, :]).astype(jnp.bfloat16)
    vb[me] = jnp.transpose(both[:, PAIR : 2 * PAIR]).astype(jnp.bfloat16)

    def split_heads(dst, query):
        low = low_half(query.shape)
        dst[0] = jnp.where(low, query, 0.0).astype(jnp.bfloat16)
        dst[1] = jnp.where(low, 0.0, query).astype(jnp.bfloat16)

    both = project(2 * PAIR, 2 * PAIR)
    for q in range(kv_parts):
        for d in (0, 1):
            if last > 0 or halfway(d, q):
                kv_copy(d, 0, q).start()
    turned = jnp.transpose(pair_norm(both[:, 0:PAIR], qk_gain_ref[2:3, :]))
    first = lax.broadcasted_iota(jnp.int32, turned.shape, 0) < HEAD
    fqb[0] = jnp.where(first, turned, 0.0).astype(jnp.bfloat16)
    fqb[1] = jnp.where(first, 0.0, turned).astype(jnp.bfloat16)
    split_heads(wqb, pair_norm(both[:, PAIR : 2 * PAIR], qk_gain_ref[0:1, :]))

    to_log2 = log2e * HEAD ** (-0.5)

    def absorb(block, own):
        scores = []
        for h in (0, 1):
            key_gate = gates[me, 0:1, h : h + 1] - gates[block, :, h : h + 1]
            both = jnp.dot(kb[block], fqb[h], preferred_element_type=jnp.float32) * to_log2 + key_gate
            if own:
                key_pos = lax.broadcasted_iota(jnp.int32, both.shape, 0)
                query_pos = lax.broadcasted_iota(jnp.int32, both.shape, 1)
                both = jnp.where(query_pos >= key_pos, both, big_negative)
            scores.append(both)
        parts = []
        for h in (0, 1):
            top = jnp.max(scores[h], axis=0, keepdims=True)
            if not own:
                before = maxb[h]
                top = jnp.maximum(before, top)
            weights = jnp.exp2(scores[h] - top)
            total = jnp.sum(weights, axis=0, keepdims=True)
            shrink = None
            if not own:
                shrink = jnp.exp2(before - top)
                total += sumb[h] * shrink
            maxb[h] = top
            sumb[h] = total
            parts.append((weights.astype(jnp.bfloat16), shrink))
        for h, (weights, shrink) in enumerate(parts):
            head = pl.ds(h * HEAD, HEAD)
            product = jnp.dot(vb[block, head], weights, preferred_element_type=jnp.float32)
            if not own:
                product += accb[head] * shrink
            accb[head] = product

    def window_project():
        raw = project(4 * PAIR, PAIR)
        low = low_half(raw.shape)
        mean = jnp.sum(jnp.where(low, raw * raw, 0.0), axis=1, keepdims=True) * (1.0 / HEAD)
        key = raw * lax.rsqrt(mean + epsilon) * qk_gain_ref[1:2, :]
        ext = jnp.where(low, key, raw)
        turned = pltpu.roll(ext, HEAD, 1)
        keys_ext[WINDOW:, :] = jnp.where(low, ext, turned).astype(jnp.bfloat16)
        values_ext[WINDOW:, :] = jnp.where(low, turned, ext).astype(jnp.bfloat16)
        prev[0] = ext[rows - WINDOW :, :].astype(jnp.bfloat16)

    def prev_copy():
        return ring_copy(prev.at[0], prev.at[1], prev_send, prev_recv, 0)

    def window_send():
        prev_copy().start()

    def window_attend():
        prev_copy().wait_recv()
        ext = prev[1].astype(jnp.float32)
        low = low_half(ext.shape)
        turned = pltpu.roll(ext, HEAD, 1)
        keys_ext[0:WINDOW, :] = jnp.where(low, ext, turned).astype(jnp.bfloat16)
        values_ext[0:WINDOW, :] = jnp.where(low, turned, ext).astype(jnp.bfloat16)
        for r in range(tiles):
            part = pl.ds(r * 128, 128)
            outs = []
            for h in (0, 1):
                span = pl.ds(r * 128, 128 + WINDOW)
                scores = dot_nt(wqb[h, part], keys_ext[span, :]) * HEAD ** (-0.5)
                distance = (
                    WINDOW
                    + lax.broadcasted_iota(jnp.int32, scores.shape, 0)
                    - lax.broadcasted_iota(jnp.int32, scores.shape, 1)
                )
                key_pos = (
                    me * rows + r * 128 - WINDOW + lax.broadcasted_iota(jnp.int32, scores.shape, 1)
                )
                valid = (distance >= 0) & (distance < WINDOW) & (key_pos >= 0)
                sink = sink_ref[h]
                top = jnp.maximum(
                    jnp.max(jnp.where(valid, scores, big_negative), axis=1, keepdims=True), sink
                )
                weights = jnp.where(valid, jnp.exp(scores - top), 0.0)
                total = jnp.sum(weights, axis=1, keepdims=True) + jnp.exp(sink - top)
                probs = (weights / total).astype(jnp.bfloat16)
                outs.append(
                    jnp.dot(probs, values_ext[span, :], preferred_element_type=jnp.float32)
                )
            merged = jnp.where(low_half(outs[0].shape), outs[0], outs[1])
            wob[t, part] = merged.astype(jnp.bfloat16)

    def merge_project(b):
        logits = project(first_merge + b * cols, cols)
        sgb[b] = jax.nn.sigmoid(logits)

    def branch_project(buf, b):
        per = n // tp
        high = depth // 2
        total = jnp.zeros((rows, cols), jnp.float32)
        for k in range(tp):
            weights = wb[k * per : (k + 1) * per, b * high : (b + 1) * high, first_branch:].reshape(
                per * high, cols
            )
            total += jnp.dot(buf[k], weights, preferred_element_type=jnp.float32)
        return total

    def window_mix():
        window_outs.finish()
        mixb[...] = sgb[0] * branch_project(wob, 0)

    absorb(me, True)
    tasks = (
        [window_project, window_send, window_attend, window_outs.begin]
        + [functools.partial(window_outs.advance, s) for s in range(window_outs.steps)]
        + [functools.partial(merge_project, b) for b in (0, 1)]
        + [window_mix]
    )

    def kv_step(s, carry):
        for q in range(kv_parts):
            for d in (0, 1):
                kv_copy(d, s - 1, q).wait_recv()
                if halfway(d, q):
                    kv_copy(d, s, q).start()
                else:
                    pl.when(s < last)(kv_copy(d, s, q).start)
        run_at(s, tasks, 1)
        pl.when(me >= s)(functools.partial(absorb, lax.rem(me + n - s, n), False))
        pl.when(me + s >= n)(functools.partial(absorb, lax.rem(me + s, n), False))
        return carry

    lax.fori_loop(1, last + 1, kv_step, 0)
    run_late(tasks, 1)
    for d in (0, 1):
        for q in range(kv_parts):
            if halfway(d, q):
                kv_copy(d, last, q).wait_recv()
    pl.when(me >= n // 2)(functools.partial(absorb, lax.rem(me + n // 2, n), False))

    for h in (0, 1):
        head = pl.ds(h * HEAD, HEAD)
        accb[head] = accb[head] / sumb[h]
    fob[t] = jnp.transpose(accb[...]).astype(jnp.bfloat16)
    forget_outs.begin()
    for s in range(forget_outs.steps):
        forget_outs.advance(s)
    forget_outs.finish()
    out_ref[...] = (mixb[...] + sgb[1] * branch_project(fob, 1)).astype(jnp.bfloat16)

    def drain_step(s, carry):
        for d in (0, 1):

            def full(d=d):
                g_copy(d, s).wait_send()
                for q in range(len(quarters)):
                    for c in (0, 1):
                        w_copy(d, s, q, c).wait_send()
                if share:
                    pair_copy(d, s).wait_send()

            if d == 0:
                full()
            else:
                pl.when(s < last)(full)
            for q in range(kv_parts):
                if halfway(d, q):
                    kv_copy(d, s, q).wait_send()
                else:
                    pl.when(s < last)(kv_copy(d, s, q).wait_send)
        return carry

    lax.fori_loop(0, last + 1, drain_step, 0)
    prev_copy().wait_send()
    for gather in (tokens, window_outs, forget_outs):
        gather.drain()


def on_device(
    n,
    tp,
    share,
    tokens,
    norm_gain,
    qk_gain,
    w_query_window,
    w_key_window,
    w_value_window,
    sink_logits,
    w_query_forget,
    w_key_forget,
    w_value_forget,
    gate_cum,
    w_merge,
    w_branch,
):
    rows, cols = tokens.shape
    depth = w_merge.shape[0]
    width = norm_gain.shape[0]
    weights = jnp.concatenate(
        [
            w_key_forget,
            w_value_forget,
            w_query_forget,
            w_query_window,
            w_key_window,
            w_value_window,
            w_merge.reshape(depth, -1),
            w_branch.reshape(depth, -1),
        ],
        axis=1,
    )
    steps, chips = n // 2, tp // 2
    tp_sems = [
        pltpu.SemaphoreType.DMA((2, max(chips // 2, 1), 2)),
        pltpu.SemaphoreType.DMA((2, max(chips // 2, 1), 2)),
        pltpu.SemaphoreType.DMA((chips,)),
        pltpu.SemaphoreType.DMA((chips,)),
    ]
    w_pieces, kv_pieces = (6 if share else 8), 4
    bf16, f32 = jnp.bfloat16, jnp.float32
    vmem = pl.BlockSpec(memory_space=pltpu.VMEM)
    return pl.pallas_call(
        functools.partial(kernel, n, tp, share),
        out_shape=jax.ShapeDtypeStruct((rows, cols), bf16),
        in_specs=[vmem] * 5 + [pl.BlockSpec(memory_space=pltpu.SMEM)],
        out_specs=vmem,
        scratch_shapes=[
            pltpu.VMEM((tp, rows, cols), bf16),
            pltpu.VMEM((rows, width), bf16),
            pltpu.VMEM((n, depth, weights.shape[1]), bf16),
            pltpu.VMEM((n, 2, rows), f32),
            pltpu.VMEM((n, rows, 128), f32),
            pltpu.VMEM((n, rows, PAIR), bf16),
            pltpu.VMEM((n, PAIR, rows), bf16),
            pltpu.VMEM((2, WINDOW, PAIR), bf16),
            pltpu.VMEM((WINDOW + rows, PAIR), bf16),
            pltpu.VMEM((WINDOW + rows, PAIR), bf16),
            pltpu.VMEM((2, rows, PAIR), bf16),
            pltpu.VMEM((2, PAIR, rows), bf16),
            pltpu.VMEM((tp, rows, PAIR), bf16),
            pltpu.VMEM((tp, rows, PAIR), bf16),
            pltpu.VMEM((2, rows, cols), f32),
            pltpu.VMEM((rows, cols), f32),
            pltpu.VMEM((PAIR, rows), f32),
            pltpu.VMEM((2, 1, rows), f32),
            pltpu.VMEM((2, 1, rows), f32),
            pltpu.SemaphoreType.DMA((2, steps, w_pieces)),
            pltpu.SemaphoreType.DMA((2, steps, w_pieces)),
            pltpu.SemaphoreType.DMA((2, steps)),
            pltpu.SemaphoreType.DMA((2, steps)),
            pltpu.SemaphoreType.DMA((2, steps)),
            pltpu.SemaphoreType.DMA((2, steps)),
            pltpu.SemaphoreType.DMA((2, steps, kv_pieces)),
            pltpu.SemaphoreType.DMA((2, steps, kv_pieces)),
            pltpu.SemaphoreType.DMA,
            pltpu.SemaphoreType.DMA,
        ]
        + tp_sems * 3,
        compiler_params=pltpu.CompilerParams(
            collective_id=0, has_side_effects=True, vmem_limit_bytes=60 * 1024 * 1024
        ),
    )(
        tokens,
        weights,
        gate_cum.T,
        norm_gain.reshape(1, width),
        jnp.concatenate([qk_gain, qk_gain], axis=1),
        sink_logits,
    )


def solution(mesh):
    return jax.shard_map(
        functools.partial(
            on_device, mesh.shape["sp"], mesh.shape["tp"], mesh.shape["grp"] % 2 == 0
        ),
        mesh=mesh,
        in_specs=(
            P(("grp", "sp"), "tp"),
            P(),
            P(),
            P("sp", "tp"),
            P("sp", "tp"),
            P("sp", "tp"),
            P("tp"),
            P("sp", "tp"),
            P("sp", "tp"),
            P("sp", "tp"),
            P(("grp", "sp"), "tp"),
            P("sp", None, "tp"),
            P(None, "sp", "tp"),
        ),
        out_specs=P(("grp", "sp"), "tp"),
        check_vma=False,
    )
```

```python
import functools
import math

import jax
import jax.numpy as jnp
from jax import lax
from jax.experimental import pallas as pl
from jax.experimental.pallas import tpu as pltpu
from jax.sharding import PartitionSpec as P

HEAD = 64
PAIR = 2 * HEAD
WINDOW = 128
MESH = pl.DeviceIdType.MESH

epsilon = 1e-06
big_negative = -1e30
log2e = math.log2(math.e)


def low_half(shape):
    return lax.broadcasted_iota(jnp.int32, shape, 1) < HEAD


def pair_norm(raw, gain):
    low = low_half(raw.shape)
    squares = raw * raw
    first = jnp.sum(jnp.where(low, squares, 0.0), axis=1, keepdims=True)
    second = jnp.sum(jnp.where(low, 0.0, squares), axis=1, keepdims=True)
    mean = jnp.where(low, first, second) * (1.0 / HEAD)
    return raw * lax.rsqrt(mean + epsilon) * gain


def dot_nt(a, b):
    return lax.dot_general(a, b, (((1,), (1,)), ((), ())), preferred_element_type=jnp.float32)


class TpGather:
    def __init__(self, source, buf, t, chips, sems):
        self.source, self.buf, self.chips = source, buf, chips
        self.send, self.recv, self.relay_send, self.relay_recv = sems
        self.t, self.x, self.core = t, t // 2, t % 2
        self.steps = chips // 2
        self.half = buf.shape[1] // 2

    def slot(self, x, core):
        return lax.rem(x + 2 * self.chips, self.chips) * 2 + core

    def block(self, d, s):
        return self.slot(self.x - s if d == 0 else self.x + s, self.core)

    def parts(self, d, s):
        return (d, 1 - d) if s < self.steps - 1 else (d,)

    def ring(self, d, s, c):
        block = self.block(d, s)
        rows = pl.ds(c * self.half, self.half)
        dst = self.buf.at[block, rows]
        src = self.source.at[rows] if s == 0 and self.source is not None else dst
        peer = self.slot(self.x + (1 if d == 0 else -1), self.core)
        return pltpu.make_async_remote_copy(
            src_ref=src,
            dst_ref=dst,
            send_sem=self.send.at[d, s, c],
            recv_sem=self.recv.at[d, s, c],
            device_id={"tp": peer},
            device_id_type=MESH,
        )

    def relay(self, k, block):
        dst = self.buf.at[block]
        src = self.source if k == 0 and self.source is not None else dst
        return pltpu.make_async_remote_copy(
            src_ref=src,
            dst_ref=dst,
            send_sem=self.relay_send.at[k],
            recv_sem=self.relay_recv.at[k],
            device_id={"tp": self.t + 1 - 2 * self.core},
            device_id_type=MESH,
        )

    def relays(self):
        order = [(0, 0)]
        for s in range(self.steps - 1):
            order += [(1 + 2 * s, -(s + 1)), (2 + 2 * s, s + 1)]
        return order + [(self.chips - 1, self.steps)]

    def begin(self):
        for d in (0, 1):
            for c in self.parts(d, 0):
                self.ring(d, 0, c).start()
        self.relay(0, self.slot(self.x, self.core)).start()

    def advance(self, s):
        for k in range(len(self.parts(0, s))):
            for d in (0, 1):
                c = self.parts(d, s)[k]
                self.ring(d, s, c).wait_recv()
                if s + 1 < self.steps and c in self.parts(d, s + 1):
                    self.ring(d, s + 1, c).start()
        if s + 1 < self.steps:
            self.relay(1 + 2 * s, self.slot(self.x - s - 1, self.core)).start()
            self.relay(2 + 2 * s, self.slot(self.x + s + 1, self.core)).start()
        else:
            self.relay(self.chips - 1, self.slot(self.x + self.steps, self.core)).start()

    def finish(self):
        for k, offset in self.relays():
            self.relay(k, self.slot(self.x + offset, 1 - self.core)).wait_recv()

    def drain(self):
        for d in (0, 1):
            for s in range(self.steps):
                for c in self.parts(d, s):
                    self.ring(d, s, c).wait_send()
        for k, offset in self.relays():
            self.relay(k, self.slot(self.x + offset, self.core)).wait_send()


def kernel(
    n,
    tp,
    share,
    tok_ref,
    w_ref,
    gate_ref,
    gain_ref,
    qk_gain_ref,
    sink_ref,
    out_ref,
    tokb,
    nb,
    wb,
    gb,
    kb,
    vb,
    prev,
    keys_ext,
    values_ext,
    wqb,
    fqb,
    fob,
    wob,
    sgb,
    mixb,
    accb,
    maxb,
    sumb,
    w_send,
    w_recv,
    pair_send,
    pair_recv,
    g_send,
    g_recv,
    kv_send,
    kv_recv,
    prev_send,
    prev_recv,
    *tp_sems,
):
    me = lax.axis_index("sp")
    t = lax.axis_index("tp")
    right, left = lax.rem(me + 1, n), lax.rem(me + n - 1, n)
    chips = tp // 2
    rows, cols = tok_ref.shape
    depth = w_ref.shape[0]
    width = gain_ref.shape[1]
    quarter = depth // 4
    group = lax.axis_index("grp")
    odd = group % 2
    quarters = [2 + odd, 0, 1] if share else [0, 1, 2, 3]
    cuts = [0, w_ref.shape[1] - 3 * tok_ref.shape[1], w_ref.shape[1]]
    last = n // 2 - 1
    tiles = rows // 128
    first_branch = w_ref.shape[1] - cols
    first_merge = first_branch - 2 * cols

    def head_gain(k):
        gain = qk_gain_ref[k : k + 1, :]
        return jnp.concatenate([gain, gain], axis=1)

    tokens = TpGather(tok_ref, tokb, t, chips, tp_sems[0:4])
    window_outs = TpGather(None, wob, t, chips, tp_sems[4:8])
    forget_outs = TpGather(None, fob, t, chips, tp_sems[8:12])

    barrier = pltpu.get_barrier_semaphore()
    greeted = [
        {"sp": right},
        {"sp": left},
        {"tp": tokens.slot(tokens.x + 1, tokens.core)},
        {"tp": tokens.slot(tokens.x - 1, tokens.core)},
        {"tp": t + 1 - 2 * tokens.core},
    ]
    if share:
        greeted.append({"grp": group + 1 - 2 * odd})
    for device in greeted:
        pl.semaphore_signal(barrier, inc=1, device_id=device, device_id_type=MESH)
    pl.semaphore_wait(barrier, len(greeted))

    def ring_block(d, s):
        return lax.rem(me + n - s, n) if d == 0 else lax.rem(me + s, n)

    def to_next(d):
        return {"sp": right if d == 0 else left}

    def ring_copy(src, dst, send, recv, d):
        return pltpu.make_async_remote_copy(
            src_ref=src,
            dst_ref=dst,
            send_sem=send,
            recv_sem=recv,
            device_id=to_next(d),
            device_id_type=MESH,
        )

    def quarter_rows(k):
        return pl.ds(k * quarter if isinstance(k, int) else pl.multiple_of(k * quarter, 16), quarter)

    def w_copy(d, s, q, c, own=False):
        rows_of, cols_of = quarter_rows(quarters[q]), pl.ds(cuts[c], cuts[c + 1] - cuts[c])
        dst = wb.at[ring_block(d, s), rows_of, cols_of]
        src = w_ref.at[rows_of, cols_of] if own else dst
        k = 2 * q + c
        return ring_copy(src, dst, w_send.at[d, s, k], w_recv.at[d, s, k], d)

    def pair_copy(d, s):
        block = wb.at[ring_block(d, s + 1), quarter_rows(quarters[0])]
        return pltpu.make_async_remote_copy(
            src_ref=block,
            dst_ref=block,
            send_sem=pair_send.at[d, s],
            recv_sem=pair_recv.at[d, s],
            device_id={"grp": group + 1 - 2 * odd},
            device_id_type=MESH,
        )

    def g_copy(d, s, own=False):
        dst = gb.at[ring_block(d, s)]
        return ring_copy(gate_ref if own else dst, dst, g_send.at[d, s], g_recv.at[d, s], d)

    kv_parts = 4

    def kv_copy(d, s, q):
        block = ring_block(d, s)
        if q % 2 == 0:
            dst = kb.at[block, pl.ds(q // 2 * (rows // 2), rows // 2)]
        else:
            dst = vb.at[block, pl.ds(q // 2 * HEAD, HEAD)]
        return ring_copy(dst, dst, kv_send.at[d, s, q], kv_recv.at[d, s, q], d)

    def halfway(d, q):
        return q // 2 == d

    for q in range(len(quarters)):
        for c in (0, 1):
            for d in (0, 1):
                if d == 0 or last > 0:
                    w_copy(d, 0, q, c, own=True).start()
    wb[me] = w_ref[...]
    gb[me] = gate_ref[...]
    tokb[t] = tok_ref[...]

    def normalize():
        tokens.finish()
        for r in range(tiles):
            part = pl.ds(r * 128, 128)
            total = jnp.zeros((128, 1), jnp.float32)
            for k in range(tp):
                x = tokb[k, part].astype(jnp.float32)
                total += jnp.sum(x * x, axis=1, keepdims=True)
            scale = lax.rsqrt(total * (1.0 / width) + epsilon)
            for k in range(tp):
                x = tokb[k, part].astype(jnp.float32)
                nb[part, k * cols : (k + 1) * cols] = (
                    x * scale * gain_ref[:, k * cols : (k + 1) * cols]
                ).astype(jnp.bfloat16)

    def run_at(step, tasks, spacing):
        for k, task in enumerate(tasks):
            at = spacing * (1 + k)
            if at <= last:
                pl.when(step == at)(task)

    def run_late(tasks, spacing):
        for k, task in enumerate(tasks):
            if spacing * (1 + k) > last:
                task()

    token_tasks = [functools.partial(tokens.advance, s) for s in range(tokens.steps)] + [normalize]
    tokens.begin()

    def w_step(s, carry):
        for q in range(len(quarters)):
            for c in (0, 1):
                for d in (0, 1):
                    w_copy(d, s - 1, q, c).wait_recv()
                    if d == 0:
                        w_copy(d, s, q, c).start()
                    else:
                        pl.when(s < last)(w_copy(d, s, q, c).start)
            if share and q == 0:
                for d in (0, 1):
                    pair_copy(d, s - 1).start()
        run_at(s, token_tasks, 3)
        return carry

    lax.fori_loop(1, last + 1, w_step, 0)
    run_late(token_tasks, 3)
    for q in range(len(quarters)):
        for c in (0, 1):
            w_copy(0, last, q, c).wait_recv()
        if share and q == 0:
            pair_copy(0, last).start()
    if share:

        def pair_step(s, carry):
            pair_copy(0, s).wait_recv()
            pl.when(s < last)(pair_copy(1, s).wait_recv)
            return carry

        lax.fori_loop(0, last + 1, pair_step, 0)

    def project(start, size):
        weights = wb[:, :, start : start + size].reshape(width, size)
        return jnp.dot(nb[...], weights, preferred_element_type=jnp.float32)

    both = project(0, 2 * PAIR)
    for d in (0, 1):
        if d == 0 or last > 0:
            g_copy(d, 0, own=True).start()
    kb[me] = pair_norm(both[:, 0:PAIR], head_gain(3)).astype(jnp.bfloat16)
    vb[me] = jnp.transpose(both[:, PAIR : 2 * PAIR]).astype(jnp.bfloat16)

    def split_heads(dst, query):
        low = low_half(query.shape)
        dst[0] = jnp.where(low, query, 0.0).astype(jnp.bfloat16)
        dst[1] = jnp.where(low, 0.0, query).astype(jnp.bfloat16)

    def kv_begin(pieces):
        for q in pieces:
            for d in (0, 1):
                if last > 0 or halfway(d, q):
                    kv_copy(d, 0, q).start()

    kv_begin((0, 2))
    both = project(2 * PAIR, 2 * PAIR)
    kv_begin((1, 3))
    turned = jnp.transpose(pair_norm(both[:, 0:PAIR], head_gain(2)))
    first = lax.broadcasted_iota(jnp.int32, turned.shape, 0) < HEAD
    fqb[0] = jnp.where(first, turned, 0.0).astype(jnp.bfloat16)
    fqb[1] = jnp.where(first, 0.0, turned).astype(jnp.bfloat16)
    split_heads(wqb, pair_norm(both[:, PAIR : 2 * PAIR], head_gain(0)))

    to_log2 = log2e * HEAD ** (-0.5)

    def absorb(block, own):
        scores = []
        relative = (gb[me][:, 0:1] - gb[block]) * log2e
        turned = jnp.transpose(jnp.concatenate([relative] * 4, axis=0))
        for h in (0, 1):
            key_gate = turned[:, h : h + 1]
            both = jnp.dot(kb[block], fqb[h], preferred_element_type=jnp.float32) * to_log2 + key_gate
            if own:
                key_pos = lax.broadcasted_iota(jnp.int32, both.shape, 0)
                query_pos = lax.broadcasted_iota(jnp.int32, both.shape, 1)
                both = jnp.where(query_pos >= key_pos, both, big_negative)
            scores.append(both)
        parts = []
        for h in (0, 1):
            top = jnp.max(scores[h], axis=0, keepdims=True)
            if not own:
                before = maxb[h]
                top = jnp.maximum(before, top)
            weights = jnp.exp2(scores[h] - top)
            total = jnp.sum(weights, axis=0, keepdims=True)
            shrink = None
            if not own:
                shrink = jnp.exp2(before - top)
                total += sumb[h] * shrink
            maxb[h] = top
            sumb[h] = total
            parts.append((weights.astype(jnp.bfloat16), shrink))
        for h, (weights, shrink) in enumerate(parts):
            head = pl.ds(h * HEAD, HEAD)
            product = jnp.dot(vb[block, head], weights, preferred_element_type=jnp.float32)
            if not own:
                product += accb[head] * shrink
            accb[head] = product

    def window_project():
        raw = project(4 * PAIR, PAIR)
        low = low_half(raw.shape)
        mean = jnp.sum(jnp.where(low, raw * raw, 0.0), axis=1, keepdims=True) * (1.0 / HEAD)
        key = raw * lax.rsqrt(mean + epsilon) * head_gain(1)
        ext = jnp.where(low, key, raw)
        turned = pltpu.roll(ext, HEAD, 1)
        keys_ext[WINDOW:, :] = jnp.where(low, ext, turned).astype(jnp.bfloat16)
        values_ext[WINDOW:, :] = jnp.where(low, turned, ext).astype(jnp.bfloat16)
        prev[0] = ext[rows - WINDOW :, :].astype(jnp.bfloat16)

    def prev_copy():
        return ring_copy(prev.at[0], prev.at[1], prev_send, prev_recv, 0)

    def window_send():
        prev_copy().start()

    def window_attend():
        prev_copy().wait_recv()
        ext = prev[1].astype(jnp.float32)
        low = low_half(ext.shape)
        turned = pltpu.roll(ext, HEAD, 1)
        keys_ext[0:WINDOW, :] = jnp.where(low, ext, turned).astype(jnp.bfloat16)
        values_ext[0:WINDOW, :] = jnp.where(low, turned, ext).astype(jnp.bfloat16)
        for r in range(tiles):
            part = pl.ds(r * 128, 128)
            outs = []
            for h in (0, 1):
                span = pl.ds(r * 128, 128 + WINDOW)
                scores = dot_nt(wqb[h, part], keys_ext[span, :]) * HEAD ** (-0.5)
                distance = (
                    WINDOW
                    + lax.broadcasted_iota(jnp.int32, scores.shape, 0)
                    - lax.broadcasted_iota(jnp.int32, scores.shape, 1)
                )
                key_pos = (
                    me * rows + r * 128 - WINDOW + lax.broadcasted_iota(jnp.int32, scores.shape, 1)
                )
                valid = (distance >= 0) & (distance < WINDOW) & (key_pos >= 0)
                sink = sink_ref[h]
                top = jnp.maximum(
                    jnp.max(jnp.where(valid, scores, big_negative), axis=1, keepdims=True), sink
                )
                weights = jnp.where(valid, jnp.exp(scores - top), 0.0)
                total = jnp.sum(weights, axis=1, keepdims=True) + jnp.exp(sink - top)
                probs = (weights / total).astype(jnp.bfloat16)
                outs.append(
                    jnp.dot(probs, values_ext[span, :], preferred_element_type=jnp.float32)
                )
            merged = jnp.where(low_half(outs[0].shape), outs[0], outs[1])
            wob[t, part] = merged.astype(jnp.bfloat16)

    def merge_project(b):
        logits = project(first_merge + b * cols, cols)
        sgb[b] = jax.nn.sigmoid(logits)

    def branch_project(buf, b):
        per = n // tp
        high = depth // 2
        total = jnp.zeros((rows, cols), jnp.float32)
        for k in range(tp):
            weights = wb[k * per : (k + 1) * per, b * high : (b + 1) * high, first_branch:].reshape(
                per * high, cols
            )
            total += jnp.dot(buf[k], weights, preferred_element_type=jnp.float32)
        return total

    def window_mix():
        window_outs.finish()
        mixb[...] = sgb[0] * branch_project(wob, 0)

    absorb(me, True)
    tasks = (
        [window_project, window_send, window_attend, window_outs.begin, lambda: None]
        + [functools.partial(window_outs.advance, s) for s in range(window_outs.steps)]
        + [functools.partial(merge_project, b) for b in (0, 1)]
        + [window_mix]
    )

    def kv_step(s, carry):
        for d in (0, 1):
            g_copy(d, s - 1).wait_recv()
            if d == 0:
                g_copy(d, s).start()
            else:
                pl.when(s < last)(g_copy(d, s).start)
        for q in range(kv_parts):
            for d in (0, 1):
                kv_copy(d, s - 1, q).wait_recv()
                if halfway(d, q):
                    kv_copy(d, s, q).start()
                else:
                    pl.when(s < last)(kv_copy(d, s, q).start)
        run_at(s, tasks, 1)
        pl.when(me >= s)(functools.partial(absorb, lax.rem(me + n - s, n), False))
        pl.when(me + s >= n)(functools.partial(absorb, lax.rem(me + s, n), False))
        return carry

    lax.fori_loop(1, last + 1, kv_step, 0)
    run_late(tasks, 1)
    g_copy(0, last).wait_recv()
    for d in (0, 1):
        for q in range(kv_parts):
            if halfway(d, q):
                kv_copy(d, last, q).wait_recv()
    pl.when(me >= n // 2)(functools.partial(absorb, lax.rem(me + n // 2, n), False))

    for h in (0, 1):
        head = pl.ds(h * HEAD, HEAD)
        accb[head] = accb[head] / sumb[h]
    fob[t] = jnp.transpose(accb[...]).astype(jnp.bfloat16)
    forget_outs.begin()
    for s in range(forget_outs.steps):
        forget_outs.advance(s)
    forget_outs.finish()
    out_ref[...] = (mixb[...] + sgb[1] * branch_project(fob, 1)).astype(jnp.bfloat16)

    def drain_step(s, carry):
        for d in (0, 1):

            def full(d=d):
                g_copy(d, s).wait_send()
                for q in range(len(quarters)):
                    for c in (0, 1):
                        w_copy(d, s, q, c).wait_send()
                if share:
                    pair_copy(d, s).wait_send()

            if d == 0:
                full()
            else:
                pl.when(s < last)(full)
            for q in range(kv_parts):
                if halfway(d, q):
                    kv_copy(d, s, q).wait_send()
                else:
                    pl.when(s < last)(kv_copy(d, s, q).wait_send)
        return carry

    lax.fori_loop(0, last + 1, drain_step, 0)
    prev_copy().wait_send()
    for gather in (tokens, window_outs, forget_outs):
        gather.drain()


def on_device(
    n,
    tp,
    share,
    tokens,
    norm_gain,
    qk_gain,
    w_query_window,
    w_key_window,
    w_value_window,
    sink_logits,
    w_query_forget,
    w_key_forget,
    w_value_forget,
    gate_cum,
    w_merge,
    w_branch,
):
    rows, cols = tokens.shape
    depth = w_merge.shape[0]
    width = norm_gain.shape[0]
    weights = jnp.concatenate(
        [
            w_key_forget,
            w_value_forget,
            w_query_forget,
            w_query_window,
            w_key_window,
            w_value_window,
            w_merge.reshape(depth, -1),
            w_branch.reshape(depth, -1),
        ],
        axis=1,
    )
    steps, chips = n // 2, tp // 2
    tp_sems = [
        pltpu.SemaphoreType.DMA((2, max(chips // 2, 1), 2)),
        pltpu.SemaphoreType.DMA((2, max(chips // 2, 1), 2)),
        pltpu.SemaphoreType.DMA((chips,)),
        pltpu.SemaphoreType.DMA((chips,)),
    ]
    w_pieces, kv_pieces = (6 if share else 8), 4
    bf16, f32 = jnp.bfloat16, jnp.float32
    vmem = pl.BlockSpec(memory_space=pltpu.VMEM)
    return pl.pallas_call(
        functools.partial(kernel, n, tp, share),
        out_shape=jax.ShapeDtypeStruct((rows, cols), bf16),
        in_specs=[vmem] * 5 + [pl.BlockSpec(memory_space=pltpu.SMEM)],
        out_specs=vmem,
        scratch_shapes=[
            pltpu.VMEM((tp, rows, cols), bf16),
            pltpu.VMEM((rows, width), bf16),
            pltpu.VMEM((n, depth, weights.shape[1]), bf16),
            pltpu.VMEM((n, 2, rows), f32),
            pltpu.VMEM((n, rows, PAIR), bf16),
            pltpu.VMEM((n, PAIR, rows), bf16),
            pltpu.VMEM((2, WINDOW, PAIR), bf16),
            pltpu.VMEM((WINDOW + rows, PAIR), bf16),
            pltpu.VMEM((WINDOW + rows, PAIR), bf16),
            pltpu.VMEM((2, rows, PAIR), bf16),
            pltpu.VMEM((2, PAIR, rows), bf16),
            pltpu.VMEM((tp, rows, PAIR), bf16),
            pltpu.VMEM((tp, rows, PAIR), bf16),
            pltpu.VMEM((2, rows, cols), f32),
            pltpu.VMEM((rows, cols), f32),
            pltpu.VMEM((PAIR, rows), f32),
            pltpu.VMEM((2, 1, rows), f32),
            pltpu.VMEM((2, 1, rows), f32),
            pltpu.SemaphoreType.DMA((2, steps, w_pieces)),
            pltpu.SemaphoreType.DMA((2, steps, w_pieces)),
            pltpu.SemaphoreType.DMA((2, steps)),
            pltpu.SemaphoreType.DMA((2, steps)),
            pltpu.SemaphoreType.DMA((2, steps)),
            pltpu.SemaphoreType.DMA((2, steps)),
            pltpu.SemaphoreType.DMA((2, steps, kv_pieces)),
            pltpu.SemaphoreType.DMA((2, steps, kv_pieces)),
            pltpu.SemaphoreType.DMA,
            pltpu.SemaphoreType.DMA,
        ]
        + tp_sems * 3,
        compiler_params=pltpu.CompilerParams(
            collective_id=0, has_side_effects=True, vmem_limit_bytes=60 * 1024 * 1024
        ),
    )(
        tokens,
        weights,
        gate_cum.T,
        norm_gain.reshape(1, width),
        qk_gain,
        sink_logits,
    )


def solution(mesh):
    return jax.shard_map(
        functools.partial(
            on_device, mesh.shape["sp"], mesh.shape["tp"], mesh.shape["grp"] % 2 == 0
        ),
        mesh=mesh,
        in_specs=(
            P(("grp", "sp"), "tp"),
            P(),
            P(),
            P("sp", "tp"),
            P("sp", "tp"),
            P("sp", "tp"),
            P("tp"),
            P("sp", "tp"),
            P("sp", "tp"),
            P("sp", "tp"),
            P(("grp", "sp"), "tp"),
            P("sp", None, "tp"),
            P(None, "sp", "tp"),
        ),
        out_specs=P(("grp", "sp"), "tp"),
        check_vma=False,
    )
```
